32 devices in a mesh: grp: 2 (over y), kv: 4 (over z), tp: 4 (over x, core).
Axes of the slice: x: 2, y: 2, z: 4, core: 2. Of those that a mesh axis runs over, the one named last changes fastest.
Arguments:
- tokens: bfloat16 [256, 4096], P('grp', 'kv'), parts along dimension 0, may hold values from -36 to 36
- span_lengths: int32 [256], P(('grp', 'kv')), parts along dimension 0, may hold values from 1 to 256, 13107 in all
- block_state: float32 [256, 64, 32, 64], P(('grp', 'kv'), 'tp'), parts along dimension 0, may hold values from -96 to 96
- key_cache: bfloat16 [256, 2048, 256], P(('grp', 'kv'), 'tp'), parts along dimension 0, may hold values from -6 to 6
- value_cache: bfloat16 [256, 4096, 256], P(('grp', 'kv'), 'tp'), parts along dimension 0, may hold values from -6 to 6
- decay_cache: float32 [256, 2048, 256], P(('grp', 'kv'), 'tp'), parts along dimension 0, may hold values from -34 to 0, as said below
- attn_gain: float32 [4096], P('kv'), may hold values from 0.1 to 1.9
- query_weight: bfloat16 [4096, 2048], P('kv', 'tp'), may hold values from -0.09375 to 0.09375
- key_weight: bfloat16 [4096, 2048], P('kv', 'tp'), may hold values from -0.09375 to 0.09375
- value_weight: bfloat16 [4096, 4096], P('kv', 'tp'), may hold values from -0.09375 to 0.09375
- gate_weight: bfloat16 [4096, 4096], P('kv', 'tp'), may hold values from -0.09375 to 0.09375
- decay_matrix: bfloat16 [4096, 2048], P('kv', 'tp'), may hold values from -0.09375 to 0.09375
- decay_offset_bias: float32 [2048], P('tp'), may hold values from -1.4 to 6
- head_gain: float32 [64], replicated, may hold values from 0.1 to 1.9
- out_weight: bfloat16 [4096, 4096], P('tp', 'kv'), may hold values from -0.09375 to 0.09375
- mixer_gain: float32 [4096], P('kv'), may hold values from 0.1 to 1.9
- up_weight: bfloat16 [4096, 16384], P('kv', 'tp'), may hold values from -0.09375 to 0.09375
- down_weight: bfloat16 [16384, 4096], P('tp', 'kv'), may hold values from -0.046875 to 0.046875
Outputs:
- layer_out: bfloat16 [256, 4096], P('grp', 'kv'), parts along dimension 0
The draws below stay inside these ranges and needn't reach their ends.
There are 2 independent parts, one for each index of `grp`. The reference program is written for one: setup_inputs(seed, part) draws one part's arguments, and reference() takes and returns one part's arrays. A program takes and returns all parts, laid end to end along the dimension named above; an argument that names none is the same for every part. Nothing has to cross between parts.
Inputs may be any that keep to these rules, and one draw needn't show every extreme that they name: Cached positions at index span_lengths - 1 and beyond are unused. `decay_cache`: Non-increasing along positions.
All inputs are finite; a program needn't handle non-finite values. No bound on the sum of `span_lengths` on one device may be relied on, other than what follows from the above.
Results may differ from the reference program's by a relative error of at most 0.005.
The reference program's roundings to bfloat16 on the way count: a program that leaves them out, or rounds other values in their place, can miss the bound.
Values may be sent and summed in bfloat16 or wider, within the bound.
A program may use at most 128 MiB of HBM per device.

```python
import math
import jax
import jax.numpy as jnp
import numpy as np
from jax import lax

D = 4096
HEAD_NUMBER = 64
KEY_WIDTH = 32
DV = 64
FF = 16384
SEQUENCE_NUMBER = 128
OPEN_POSITIONS = 256


def draw_tokens(key, part):
    key_base, key_rows = jax.random.split(jax.random.fold_in(key, 11))
    column = jnp.arange(D, dtype=jnp.float32) / (D - 1)
    base = jax.random.truncated_normal(key_base, -4.0, 4.0, (SEQUENCE_NUMBER, D), jnp.float32)
    column_scale = jnp.exp(math.log(0.3) + column * math.log(10.0))
    scale_per_row = jnp.exp(jax.random.uniform(key_rows, (SEQUENCE_NUMBER, 1), jnp.float32, math.log(0.3), math.log(3.0)))
    return (base * column_scale * scale_per_row).astype(jnp.bfloat16)


def draw_decay_offset_bias(key, part):
    key_head, key_fast, key_slow = jax.random.split(jax.random.fold_in(key, 23), 3)
    fast_share = 0.5
    fast_head = jax.random.uniform(key_head, (HEAD_NUMBER,), jnp.float32) < fast_share
    fast_channel = jnp.repeat(fast_head, KEY_WIDTH)
    fast_value = jax.random.uniform(key_fast, (HEAD_NUMBER * KEY_WIDTH,), jnp.float32, -1.4, 0.4)
    slow_value = jax.random.uniform(key_slow, (HEAD_NUMBER * KEY_WIDTH,), jnp.float32, 3.0, 6.0)
    return jnp.where(fast_channel, fast_value, slow_value).astype(jnp.float32)


def draw_decay_cache(key, part):
    every_key_rows = jax.random.split(jax.random.fold_in(key, 37), 7)
    fast_share = 0.5
    fast_head = jax.random.uniform(every_key_rows[0], (SEQUENCE_NUMBER, HEAD_NUMBER), jnp.float32) < fast_share
    fast_channel = jnp.repeat(fast_head, KEY_WIDTH, axis=1)
    fast_rate = jnp.exp(jax.random.uniform(every_key_rows[1], (SEQUENCE_NUMBER, HEAD_NUMBER * KEY_WIDTH), jnp.float32, math.log(1.0 / 80.0), math.log(1.0 / 30.0)))
    slow_rate = jnp.exp(jax.random.uniform(every_key_rows[2], (SEQUENCE_NUMBER, HEAD_NUMBER * KEY_WIDTH), jnp.float32, math.log(0.1), math.log(0.5))) / OPEN_POSITIONS
    sequence_factor = jnp.exp(jax.random.uniform(every_key_rows[3], (SEQUENCE_NUMBER, 1), jnp.float32, math.log(0.5), math.log(2.0)))
    rate = jnp.where(fast_channel, fast_rate, slow_rate) * sequence_factor
    every_step_index = -rate[:, :, None] * jax.random.uniform(every_key_rows[4], (SEQUENCE_NUMBER, HEAD_NUMBER * KEY_WIDTH, OPEN_POSITIONS), jnp.float32, 0.5, 1.5)
    token_group_start = jax.random.randint(every_key_rows[5], (SEQUENCE_NUMBER, HEAD_NUMBER, 2), 0, OPEN_POSITIONS)
    token_group_length = jax.random.uniform(every_key_rows[6], (SEQUENCE_NUMBER, HEAD_NUMBER, 2), jnp.float32, math.log(0.6), math.log(0.8))
    token_place = jnp.arange(OPEN_POSITIONS, dtype=jnp.int32)
    token_group = jnp.sum(jnp.where(token_group_start[..., None] == token_place, token_group_length[..., None], 0.0), axis=2)
    token_group = jnp.repeat(token_group, KEY_WIDTH, axis=1)
    return jnp.cumsum(every_step_index + token_group, axis=-1).astype(jnp.float32)


def levels(rng, extent, pieces, smallest, high):
    factor_of = 1.0
    for dim, parts in pieces:
        heights = jax.random.uniform(jax.random.fold_in(jax.random.fold_in(rng, 6), dim), (parts,), jnp.float32, smallest / len(pieces), high / len(pieces))
        factor_of = factor_of * jnp.repeat(jnp.exp(heights), extent[dim] // parts).reshape((-1,) + (1,) * (len(extent) - 1 - dim))
    return factor_of


def length_profile(count, total, bound, skew):
    weights = [(1 << 20) // math.isqrt(rank ** skew) + 1 for rank in range(2, count + 1)]
    spare, given = total - bound - (count - 1), [1] * (count - 1)
    while spare > 0:
        candidates = [i for i in range(count - 1) if given[i] < bound]
        whole, budget = sum([weights[i] for i in candidates]), spare
        for i in candidates:
            extra = min(bound - given[i], max(1, budget * weights[i] // whole), spare)
            given[i] = given[i] + extra
            spare = spare - extra
    return np.array([bound] + given)


def uneven_parts(rng, number_of, total, bound, skew):
    if number_of == 2:
        one = jax.random.randint(rng, (), max(1, total - bound), min(bound, total - 1) + 1)
        return jnp.stack([one, total - one])
    tallies = jnp.asarray(length_profile(number_of, total, bound, skew), jnp.int32)
    couples = (number_of - 1) // 2
    donor, taker = tallies[1:1 + 2 * couples:2], tallies[2:2 + 2 * couples:2]
    room = jnp.minimum(donor - 1, bound - taker)
    moved = jax.random.randint(jax.random.fold_in(rng, 1), (couples,), 0, 1 << 20) % (room + 1)
    tallies = tallies.at[1:1 + 2 * couples:2].set(donor - moved).at[2:2 + 2 * couples:2].set(taker + moved)
    return tallies[jax.random.permutation(jax.random.fold_in(rng, 2), number_of)]


def noise(stream_key, dims, spread, reach, shards=(), kind=jnp.bfloat16):
    entries = spread * jax.random.normal(stream_key, dims, jnp.float32)
    if shards:
        entries = entries * levels(stream_key, dims, shards, -0.22, 0.18)
    return jnp.clip(entries, -reach, reach).astype(kind)


def setup_inputs(seed: int = 0, part: int = 0) -> dict:
    key_list = jax.random.split(jax.random.key(seed), 19)
    part_keys = jax.random.split(jax.random.fold_in(key_list[18], part), 19)
    return {
        "tokens": draw_tokens(jax.random.fold_in(jax.random.fold_in(key_list[18], part), 71), part),
        "span_lengths": uneven_parts(part_keys[1], SEQUENCE_NUMBER, SEQUENCE_NUMBER * OPEN_POSITIONS * 2 // 5, OPEN_POSITIONS, 2).astype(jnp.int32),
        "block_state": noise(part_keys[2], (SEQUENCE_NUMBER, HEAD_NUMBER, KEY_WIDTH, DV), 16.0, 96.0, ((0, 4), (1, 4)), jnp.float32),
        "key_cache": noise(part_keys[3], (SEQUENCE_NUMBER, HEAD_NUMBER * KEY_WIDTH, OPEN_POSITIONS), 1.0, 6.0, ((0, 4), (1, 4))),
        "value_cache": noise(part_keys[4], (SEQUENCE_NUMBER, HEAD_NUMBER * DV, OPEN_POSITIONS), 1.0, 6.0, ((0, 4), (1, 4))),
        "decay_cache": draw_decay_cache(jax.random.fold_in(jax.random.fold_in(key_list[18], part), 71), part),
        "attn_gain": jnp.clip(1.0 + 0.18 * jax.random.normal(key_list[6], (D,), jnp.float32), 0.1, 1.9),
        "query_weight": noise(key_list[7], (D, HEAD_NUMBER * KEY_WIDTH), D ** -0.5, 0.09375, ((0, 4), (1, 4))),
        "key_weight": noise(key_list[8], (D, HEAD_NUMBER * KEY_WIDTH), D ** -0.5, 0.09375, ((0, 4), (1, 4))),
        "value_weight": noise(key_list[9], (D, HEAD_NUMBER * DV), D ** -0.5, 0.09375, ((0, 4), (1, 4))),
        "gate_weight": noise(key_list[10], (D, HEAD_NUMBER * DV), D ** -0.5, 0.09375, ((0, 4), (1, 4))),
        "decay_matrix": noise(key_list[11], (D, HEAD_NUMBER * KEY_WIDTH), D ** -0.5, 0.09375, ((0, 4), (1, 4))),
        "decay_offset_bias": draw_decay_offset_bias(jax.random.fold_in(key_list[18], 71), part),
        "head_gain": jnp.clip(1.0 + 0.18 * jax.random.normal(key_list[13], (DV,), jnp.float32), 0.1, 1.9),
        "out_weight": noise(key_list[14], (HEAD_NUMBER * DV, D), (HEAD_NUMBER * DV) ** -0.5, 0.09375, ((0, 4), (1, 4))),
        "mixer_gain": jnp.clip(1.0 + 0.18 * jax.random.normal(key_list[15], (D,), jnp.float32), 0.1, 1.9),
        "up_weight": noise(key_list[16], (D, FF), D ** -0.5, 0.09375, ((0, 4), (1, 4))),
        "down_weight": noise(key_list[17], (FF, D), FF ** -0.5, 0.046875, ((0, 4), (1, 4))),
    }


NORM_EPS = 1e-06
DECAY_SOFTNESS = 16.0

def span_attend(inputs):
    query, logarithm_decay, keys_span, values_span, decays_span, start_state, length, key_new, value_new = inputs
    token_place = jnp.arange(OPEN_POSITIONS, dtype=jnp.int32)
    previous = lax.optimization_barrier(jnp.sum(jnp.where(token_place[None, None, :] == length - 2, decays_span, 0.0), axis=-1))
    now_decay = previous + logarithm_decay
    in_use = (token_place < length - 1)[None, None, :]
    factor = jnp.where(in_use, jnp.exp(now_decay[:, :, None] - decays_span), 0.0)
    scores = lax.optimization_barrier(jnp.sum(query[:, :, None] * keys_span.astype(jnp.float32) * factor, axis=1))
    rounded = lax.optimization_barrier(scores.astype(jnp.bfloat16)).astype(jnp.float32)
    history = jnp.einsum('hs,hvs->hv', rounded, values_span.astype(jnp.float32))
    carried = jnp.einsum('hc,hcv->hv', query * jnp.exp(now_decay), start_state, precision=lax.Precision.HIGHEST)
    own_term = lax.optimization_barrier(jnp.sum(query * key_new, axis=-1, keepdims=True)) * value_new
    return carried + history + own_term

def reference(tokens, span_lengths, block_state, key_cache, value_cache, decay_cache, attn_gain, query_weight, key_weight, value_weight, gate_weight, decay_matrix, decay_offset_bias, head_gain, out_weight, mixer_gain, up_weight, down_weight):
    whole_rows = tokens.astype(jnp.float32)
    mean_square = lax.optimization_barrier(jnp.mean(whole_rows * whole_rows, axis=1, keepdims=True))
    scale_per_row = lax.rsqrt(mean_square + NORM_EPS)
    scaled = (whole_rows * attn_gain).astype(jnp.bfloat16)

    def apply_projection(weight):
        return jnp.dot(scaled, weight, preferred_element_type=jnp.float32) * scale_per_row
    query = apply_projection(query_weight) * KEY_WIDTH ** (-0.5)
    key_new = apply_projection(key_weight)
    value_new = apply_projection(value_weight)
    gate = apply_projection(gate_weight)
    logarithm_decay = jax.nn.log_sigmoid(apply_projection(decay_matrix) + decay_offset_bias) / DECAY_SOFTNESS
    raw = lax.map(span_attend, (query.reshape(SEQUENCE_NUMBER, HEAD_NUMBER, KEY_WIDTH), logarithm_decay.reshape(SEQUENCE_NUMBER, HEAD_NUMBER, KEY_WIDTH), key_cache.reshape(SEQUENCE_NUMBER, HEAD_NUMBER, KEY_WIDTH, OPEN_POSITIONS), value_cache.reshape(SEQUENCE_NUMBER, HEAD_NUMBER, DV, OPEN_POSITIONS), decay_cache.reshape(SEQUENCE_NUMBER, HEAD_NUMBER, KEY_WIDTH, OPEN_POSITIONS), block_state, span_lengths.astype(jnp.int32), key_new.reshape(SEQUENCE_NUMBER, HEAD_NUMBER, KEY_WIDTH), value_new.reshape(SEQUENCE_NUMBER, HEAD_NUMBER, DV)))
    normed = raw * lax.rsqrt(lax.optimization_barrier(jnp.mean(raw * raw, axis=-1, keepdims=True)) + NORM_EPS) * head_gain
    mixed = (normed.reshape(SEQUENCE_NUMBER, HEAD_NUMBER * DV) * jax.nn.silu(gate)).astype(jnp.bfloat16)
    attn_out = jnp.dot(mixed, out_weight, preferred_element_type=jnp.float32)
    resid = (whole_rows + attn_out).astype(jnp.bfloat16)
    resid_rows = resid.astype(jnp.float32)
    mixer_square = lax.optimization_barrier(jnp.mean(resid_rows * resid_rows, axis=1, keepdims=True))
    mixer_scaled = (resid_rows * mixer_gain).astype(jnp.bfloat16)
    before = jnp.dot(mixer_scaled, up_weight, preferred_element_type=jnp.float32) * lax.rsqrt(mixer_square + NORM_EPS)
    hidden = jnp.square(jax.nn.relu(before)).astype(jnp.bfloat16)
    return (resid_rows + jnp.dot(hidden, down_weight, preferred_element_type=jnp.float32)).astype(jnp.bfloat16)
```

```python
import functools

import jax
import jax.numpy as jnp
from jax import lax
from jax.experimental import pallas as pl
from jax.experimental.pallas import tpu as pltpu
from jax.sharding import PartitionSpec as P

D = 4096
KEY_WIDTH = 32
DV = 64


NORM_EPS = 1e-06
DECAY_SOFTNESS = 16.0
MESH = pl.DeviceIdType.MESH
LANES = 128
F32 = jnp.float32
BF16 = jnp.bfloat16


def greet(axes):
    barrier = pltpu.get_barrier_semaphore()
    count = 0
    for axis in axes:
        size = lax.axis_size(axis)
        me = lax.axis_index(axis)
        for step in range(1, size):
            pl.semaphore_signal(
                barrier, inc=1, device_id={axis: lax.rem(me + step, size)}, device_id_type=MESH
            )
        count += size - 1
    pl.semaphore_wait(barrier, count)


def send(axis, step, src, dst, send_sem, recv_sem):
    size = lax.axis_size(axis)
    peer = lax.rem(lax.axis_index(axis) + step, size)
    copy = pltpu.make_async_remote_copy(
        src_ref=src(peer),
        dst_ref=dst,
        send_sem=send_sem,
        recv_sem=recv_sem,
        device_id={axis: peer},
        device_id_type=MESH,
    )
    copy.start()
    return copy


def project_kernel(
    parts, tok_ref, gain_ref, *refs
):
    weights, refs = refs[:5], refs[5:]
    sum_ref, sq_ref = refs[:2]
    wbuf, part, outgoing, incoming, sq_out, sq_in, wsem, ssem, rsem, qssem, qrsem = refs[2:]
    n, rows = outgoing.shape[0], outgoing.shape[1]
    me = lax.axis_index("kv")
    loads = []
    for i, (which, col, place, width) in enumerate(parts):
        load = pltpu.make_async_copy(
            weights[which].at[:, pl.ds(col, width)], wbuf.at[:, pl.ds(place, width)], wsem.at[i]
        )
        load.start()
        loads.append(load)
    x = tok_ref[...].astype(F32)
    scaled = (x * gain_ref[...]).astype(BF16)
    square = jnp.sum(x * x, axis=1, keepdims=True)
    sq_out[...] = jnp.broadcast_to(square, (x.shape[0], LANES)).reshape(sq_out.shape)
    greet(("kv",))
    copies = []
    for k in range(1, n):
        copies.append(
            send("kv", k, lambda p: sq_out.at[p], sq_in.at[k - 1], qssem.at[k - 1], qrsem.at[k - 1])
        )
    for i, (which, col, place, width) in enumerate(parts):
        loads[i].wait()
        cols = pl.ds(place, width)
        got = jnp.dot(scaled, wbuf[:, cols], preferred_element_type=F32).reshape(n, rows, width)
        part[:, :, cols] = got
        outgoing[:, :, cols] = got.astype(BF16)
        for k in SEND_ORDER(n):
            copies.append(
                send(
                    "kv",
                    k,
                    lambda p: outgoing.at[p, :, cols],
                    incoming.at[k - 1, :, cols],
                    ssem.at[k - 1, i],
                    rsem.at[k - 1, i],
                )
            )
    for copy in copies:
        copy.wait_recv()
    total = part[me]
    square = sq_out[me]
    for k in range(n - 1):
        total = total + incoming[k].astype(F32)
        square = square + sq_in[k]
    sum_ref[...] = total
    sq_ref[...] = square
    for copy in copies:
        copy.wait_send()


def SEND_ORDER(n):
    return sorted(range(1, n), key=lambda k: -min(k, n - k))


def project(tokens, gain, weights):
    n = lax.axis_size("kv")
    rows = tokens.shape[0] // n
    parts, place = [], 0
    for which, w in enumerate(weights):
        width = min(512, w.shape[1])
        for col in range(0, w.shape[1], width):
            parts.append((which, col, place, width))
            place += width
    vmem = pl.BlockSpec(memory_space=pltpu.VMEM)
    return pl.pallas_call(
        functools.partial(project_kernel, parts),
        out_shape=(
            jax.ShapeDtypeStruct((rows, place), F32),
            jax.ShapeDtypeStruct((rows, LANES), F32),
        ),
        in_specs=[vmem, vmem] + [pl.BlockSpec(memory_space=pltpu.HBM)] * 5,
        out_specs=(vmem, vmem),
        scratch_shapes=[
            pltpu.VMEM((tokens.shape[1], place), BF16),
            pltpu.VMEM((n, rows, place), F32),
            pltpu.VMEM((n, rows, place), BF16),
            pltpu.VMEM((n - 1, rows, place), BF16),
            pltpu.VMEM((n, rows, LANES), F32),
            pltpu.VMEM((n - 1, rows, LANES), F32),
            pltpu.SemaphoreType.DMA((len(parts),)),
            pltpu.SemaphoreType.DMA((n - 1, len(parts))),
            pltpu.SemaphoreType.DMA((n - 1, len(parts))),
            pltpu.SemaphoreType.DMA((n - 1,)),
            pltpu.SemaphoreType.DMA((n - 1,)),
        ],
        compiler_params=pltpu.CompilerParams(
            collective_id=0, has_side_effects=True, vmem_limit_bytes=40 << 20
        ),
        name="project",
    )(tokens, gain.reshape(1, -1), *weights)


NT = (((1,), (1,)), ((), ()))


def attend_kernel(
    len_ref, last_ref, sum_ref, sq_ref, bias_ref, hg_ref, k1, k2, d1, d2, v1, v2, st,
    out_ref, q_t, ld_t, qk_t, vn, gs, now_s, hist, raw,
):
    step = pl.program_id(0)
    rows = out_ref.shape[0]
    heads = st.shape[1]
    keys, vals = heads * KEY_WIDTH, heads * DV
    lane = lax.broadcasted_iota(jnp.int32, (1, LANES), 1)

    @pl.when(step == 0)
    def _():
        scale = lax.rsqrt(sq_ref[:, :1] / D + NORM_EPS)
        q = sum_ref[:, :keys] * scale * KEY_WIDTH ** (-0.5)
        key_new = sum_ref[:, keys : 2 * keys] * scale
        at = 2 * keys
        vn[...] = sum_ref[:, at : at + vals] * scale
        g = sum_ref[:, at + vals : at + 2 * vals] * scale
        gs[...] = g * (1.0 / (1.0 + jnp.exp(-g))) * jnp.concatenate([hg_ref[...]] * heads, axis=1)
        x = sum_ref[:, at + 2 * vals :] * scale + bias_ref[...]
        ld = (jnp.minimum(x, 0.0) - jnp.log1p(jnp.exp(-jnp.abs(x)))) / DECAY_SOFTNESS
        spare = jnp.zeros((LANES - rows, keys), F32)
        q_t[...] = jnp.concatenate([q, spare], axis=0).T
        ld_t[...] = jnp.concatenate([ld, spare], axis=0).T
        pick = lax.broadcasted_iota(jnp.int32, (heads, keys), 1) // KEY_WIDTH
        pick = (pick == lax.broadcasted_iota(jnp.int32, (heads, keys), 0)).astype(F32)
        qk_t[...] = lax.dot_general(
            pick,
            jnp.concatenate([q * key_new, spare], axis=0),
            NT,
            precision=lax.Precision.HIGHEST,
            preferred_element_type=F32,
        )

    length = len_ref[step]
    two = length - 1 > LANES
    mine = lane == step
    own_decay = jnp.where(mine, ld_t[...], 0.0)

    @pl.when(two)
    def _():
        prev = jnp.where(lane + LANES == length - 2, d2[0], 0.0)
        col = jnp.sum(own_decay + prev, axis=1, keepdims=True)
        now_s[...] = jnp.broadcast_to(col, now_s.shape)

    @pl.when(jnp.logical_not(two))
    def _():
        prev = jnp.where(lane == length - 2, d1[0], 0.0)
        col = jnp.sum(own_decay + prev, axis=1, keepdims=True)
        now_s[...] = jnp.broadcast_to(col, now_s.shape)

    now = now_s[...]
    q = jnp.broadcast_to(
        jnp.sum(jnp.where(mine, q_t[...], 0.0), axis=1, keepdims=True), now.shape
    )

    def block(k_ref, d_ref, v_ref, offset):
        s = k_ref[0].astype(F32) * q * jnp.exp(now - d_ref[0])
        s = jnp.sum(s.reshape(heads, KEY_WIDTH, LANES), axis=1)
        s = jnp.where(lane + offset < length - 1, s, 0.0).astype(BF16)
        return lax.dot_general(s, v_ref[0], NT, preferred_element_type=F32)

    hist[...] = block(k1, d1, v1, 0)

    @pl.when(two)
    def _():
        hist[...] += block(k2, d2, v2, LANES)

    weight = (q * jnp.exp(now))[:, :DV]
    carried = jnp.sum((weight * st[0].reshape(keys, DV)).reshape(heads, KEY_WIDTH, DV), axis=1)
    carried = jnp.concatenate([carried] * heads, axis=1)
    qk = jnp.sum(jnp.where(mine, qk_t[...], 0.0), axis=1, keepdims=True)
    whole = hist[...] + carried + qk * vn[pl.ds(step, 1), :]
    own = lax.broadcasted_iota(jnp.int32, (heads, vals), 1) // DV
    own = own == lax.broadcasted_iota(jnp.int32, (heads, vals), 0)
    whole = jnp.where(own, whole, 0.0)
    mean = jnp.sum(whole * whole, axis=1, keepdims=True) / DV
    whole = whole * lax.rsqrt(mean + NORM_EPS)
    raw[pl.ds(step, 1), :] = jnp.sum(whole, axis=0, keepdims=True)

    @pl.when(step == rows - 1)
    def _():
        out_ref[...] = (raw[...] * gs[...]).astype(BF16)


def attend(span_lengths, sums, square, bias, head_gain, keys, values, decays, state):
    rows, heads = state.shape[:2]
    kw, vw = heads * KEY_WIDTH, heads * DV
    order = jnp.arange(rows, dtype=jnp.int32)
    needed = jnp.where(span_lengths - 1 > LANES, order, 0)
    last = jnp.max(jnp.where(order[None, :] <= order[:, None], needed[None, :], 0), axis=1)

    def first(width):
        return pl.BlockSpec((1, width, LANES), lambda i, ln, la: (i, 0, 0))

    def second(width):
        return pl.BlockSpec((1, width, LANES), lambda i, ln, la: (la[i], 0, 1))

    def fixed(shape):
        return pl.BlockSpec(shape, lambda i, ln, la: (0,) * len(shape))

    return pl.pallas_call(
        attend_kernel,
        out_shape=jax.ShapeDtypeStruct((rows, vw), BF16),
        grid_spec=pltpu.PrefetchScalarGridSpec(
            num_scalar_prefetch=2,
            grid=(rows,),
            in_specs=[
                fixed(sums.shape),
                fixed(square.shape),
                fixed((1, kw)),
                fixed((1, DV)),
                first(kw),
                second(kw),
                first(kw),
                second(kw),
                first(vw),
                second(vw),
                pl.BlockSpec((1, heads, KEY_WIDTH, DV), lambda i, ln, la: (i, 0, 0, 0)),
            ],
            out_specs=fixed((rows, vw)),
            scratch_shapes=[
                pltpu.VMEM((kw, LANES), F32),
                pltpu.VMEM((kw, LANES), F32),
                pltpu.VMEM((heads, LANES), F32),
                pltpu.VMEM((rows, vw), F32),
                pltpu.VMEM((rows, vw), F32),
                pltpu.VMEM((kw, LANES), F32),
                pltpu.VMEM((heads, vw), F32),
                pltpu.VMEM((rows, vw), F32),
            ],
        ),
        compiler_params=pltpu.CompilerParams(
            dimension_semantics=("arbitrary",), vmem_limit_bytes=40 << 20
        ),
        name="attend",
    )(
        span_lengths, last, sums, square, bias.reshape(1, -1), head_gain.reshape(1, -1),
        keys, keys, decays, decays, values, values, state,
    )


def finish_kernel(
    mixed_ref, tok_ref, gain_ref, ow_ref, uw_ref, dw_ref, out_ref,
    ow, uw, dw, gath, part, t_out, t_in, resid, scaled, sq_out, sq_in,
    u_part, u_own, u_out, u_in, hid, total, t_out2, t_in2, done,
    wsem, g_s, g_r, a_s, a_r, b_s, b_r, q_s, q_r, u_s, u_r, h_s, h_r, c_s, c_r, e_s, e_r,
):
    n, m = lax.axis_size("kv"), lax.axis_size("tp")
    me, col = lax.axis_index("kv"), lax.axis_index("tp")
    chunks = u_s.shape[1]
    width = u_out.shape[2] // chunks
    loads = [
        pltpu.make_async_copy(ow_ref, ow, wsem.at[0]),
    ]
    for c in range(chunks):
        at = pl.ds(c * width, width)
        loads.append(pltpu.make_async_copy(uw_ref.at[:, at], uw.at[:, at], wsem.at[1 + c]))
    loads.append(pltpu.make_async_copy(dw_ref, dw, wsem.at[1 + chunks]))
    for load in loads:
        load.start()
    greet(("kv", "tp"))
    copies = []

    def wait_all(group):
        for copy in group:
            copy.wait_recv()
        copies.extend(group)

    group = [
        send("kv", k, lambda p: mixed_ref, gath.at[me], g_s.at[k - 1], g_r.at[k - 1])
        for k in SEND_ORDER(n)
    ]
    gath[me] = mixed_ref[...]
    wait_all(group)
    loads[0].wait()
    rows = gath.shape[0] * gath.shape[1]

    def over_tp(value, outgoing, incoming, ss, rs):
        part[...] = value.reshape(part.shape)
        outgoing[...] = value.reshape(part.shape).astype(BF16)
        group = [
            send("tp", k, lambda p: outgoing.at[p], incoming.at[k - 1], ss.at[k - 1], rs.at[k - 1])
            for k in range(1, m)
        ]
        wait_all(group)
        result = part[col]
        for k in range(m - 1):
            result = result + incoming[k].astype(F32)
        return result

    def to_tp(buffer, ss, rs):
        group = [
            send("tp", k, lambda p: buffer.at[col], buffer.at[col], ss.at[k - 1], rs.at[k - 1])
            for k in range(1, m)
        ]
        wait_all(group)

    x = gath[...].reshape(rows, gath.shape[2])
    attn = over_tp(jnp.dot(x, ow[...], preferred_element_type=F32), t_out, t_in, a_s, a_r)
    resid[col] = (tok_ref[col].astype(F32) + attn).astype(BF16)
    to_tp(resid, b_s, b_r)
    whole = resid[...].reshape(rows, resid.shape[2]).astype(F32)
    square = jnp.sum(whole * whole, axis=1, keepdims=True)
    sq_out[...] = jnp.broadcast_to(square, (rows, LANES)).reshape(sq_out.shape)
    sq_group = [
        send("kv", k, lambda p: sq_out.at[p], sq_in.at[k - 1], q_s.at[k - 1], q_r.at[k - 1])
        for k in SEND_ORDER(n)
    ]
    scaled[...] = (whole * gain_ref[...]).astype(BF16)
    groups = []
    for c in range(chunks):
        at = pl.ds(c * width, width)
        loads[1 + c].wait()
        got = jnp.dot(scaled[...], uw[:, at], preferred_element_type=F32)
        got = got.reshape(u_part.shape)
        u_part[...] = got
        u_out[:, :, at] = got.astype(BF16)
        groups.append(
            [
                send(
                    "kv", k, lambda p: u_out.at[p, :, at], u_in.at[k - 1, :, at],
                    u_s.at[k - 1, c], u_r.at[k - 1, c],
                )
                for k in SEND_ORDER(n)
            ]
        )
        u_own[:, at] = u_part[me]
    wait_all(sq_group)
    square = sq_out[me]
    for k in range(n - 1):
        square = square + sq_in[k]
    scale = lax.rsqrt(square[:, :1] / D + NORM_EPS)
    hidden_groups = []
    for c in range(chunks):
        at = pl.ds(c * width, width)
        wait_all(groups[c])
        got = u_own[:, at]
        for k in range(n - 1):
            got = got + u_in[k, :, at].astype(F32)
        hid[me, :, at] = jnp.square(jnp.maximum(got * scale, 0.0)).astype(BF16)
        hidden_groups.append(
            [
                send(
                    "kv", k, lambda p: hid.at[me, :, at], hid.at[me, :, at],
                    h_s.at[k - 1, c], h_r.at[k - 1, c],
                )
                for k in SEND_ORDER(n)
            ]
        )
    loads[1 + chunks].wait()
    for c in range(chunks):
        at = pl.ds(c * width, width)
        wait_all(hidden_groups[c])
        got = jnp.dot(
            hid[:, :, at].reshape(rows, width), dw[at, :], preferred_element_type=F32
        )
        if c == 0:
            total[...] = got
        else:
            total[...] += got
    mixer = over_tp(total[...], t_out2, t_in2, c_s, c_r)
    done[col] = (resid[col].astype(F32) + mixer).astype(BF16)
    to_tp(done, e_s, e_r)
    out_ref[...] = done[...]
    for copy in copies:
        copy.wait_send()


def finish(mixed, tokens, gain, out_weight, up_weight, down_weight):
    n, m = lax.axis_size("kv"), lax.axis_size("tp")
    rows, feats = tokens.shape
    vals, hidden = out_weight.shape[0], up_weight.shape[1]
    own, share = rows // n, rows // m
    chunks = 4
    vmem = pl.BlockSpec(memory_space=pltpu.VMEM)
    hbm = pl.BlockSpec(memory_space=pltpu.HBM)
    dma = pltpu.SemaphoreType.DMA
    out = pl.pallas_call(
        finish_kernel,
        out_shape=jax.ShapeDtypeStruct((m, share, feats), BF16),
        in_specs=[vmem, vmem, vmem, hbm, hbm, hbm],
        out_specs=vmem,
        scratch_shapes=[
            pltpu.VMEM(out_weight.shape, BF16),
            pltpu.VMEM(up_weight.shape, BF16),
            pltpu.VMEM(down_weight.shape, BF16),
            pltpu.VMEM((n, own, vals), BF16),
            pltpu.VMEM((m, share, feats), F32),
            pltpu.VMEM((m, share, feats), BF16),
            pltpu.VMEM((m - 1, share, feats), BF16),
            pltpu.VMEM((m, share, feats), BF16),
            pltpu.VMEM((rows, feats), BF16),
            pltpu.VMEM((n, own, LANES), F32),
            pltpu.VMEM((n - 1, own, LANES), F32),
            pltpu.VMEM((n, own, hidden // chunks), F32),
            pltpu.VMEM((own, hidden), F32),
            pltpu.VMEM((n, own, hidden), BF16),
            pltpu.VMEM((n - 1, own, hidden), BF16),
            pltpu.VMEM((n, own, hidden), BF16),
            pltpu.VMEM((rows, feats), F32),
            pltpu.VMEM((m, share, feats), BF16),
            pltpu.VMEM((m - 1, share, feats), BF16),
            pltpu.VMEM((m, share, feats), BF16),
            dma((2 + chunks,)),
            dma((n - 1,)),
            dma((n - 1,)),
            dma((m - 1,)),
            dma((m - 1,)),
            dma((m - 1,)),
            dma((m - 1,)),
            dma((n - 1,)),
            dma((n - 1,)),
            dma((n - 1, chunks)),
            dma((n - 1, chunks)),
            dma((n - 1, chunks)),
            dma((n - 1, chunks)),
            dma((m - 1,)),
            dma((m - 1,)),
            dma((m - 1,)),
            dma((m - 1,)),
        ],
        compiler_params=pltpu.CompilerParams(
            collective_id=1, has_side_effects=True, vmem_limit_bytes=48 << 20
        ),
        name="finish",
    )(
        mixed, tokens.reshape(m, share, feats), gain.reshape(1, -1),
        out_weight, up_weight, down_weight,
    )
    return out.reshape(rows, feats)


def kernel_shards(
    tokens,
    span_lengths,
    block_state,
    key_cache,
    value_cache,
    decay_cache,
    attn_gain,
    query_weight,
    key_weight,
    value_weight,
    gate_weight,
    decay_matrix,
    decay_offset_bias,
    head_gain,
    out_weight,
    mixer_gain,
    up_weight,
    down_weight,
):
    weights = (query_weight, key_weight, value_weight, gate_weight, decay_matrix)
    sums, square = project(tokens, attn_gain, weights)
    mixed = attend(
        span_lengths, sums, square, decay_offset_bias, head_gain,
        key_cache, value_cache, decay_cache, block_state,
    )
    return finish(mixed, tokens, mixer_gain, out_weight, up_weight, down_weight)


def fits(tokens, block_state, key_cache):
    rows, heads = block_state.shape[:2]
    share = tokens.shape[0] // lax.axis_size("tp")
    return (
        rows % 16 == 0
        and share % 16 == 0
        and heads % 8 == 0
        and rows < LANES
        and key_cache.shape[2] == 2 * LANES
    )


def shards(
    tokens,
    span_lengths,
    block_state,
    key_cache,
    value_cache,
    decay_cache,
    attn_gain,
    query_weight,
    key_weight,
    value_weight,
    gate_weight,
    decay_matrix,
    decay_offset_bias,
    head_gain,
    out_weight,
    mixer_gain,
    up_weight,
    down_weight,
):
    if fits(tokens, block_state, key_cache):
        return kernel_shards(
            tokens, span_lengths, block_state, key_cache, value_cache, decay_cache,
            attn_gain, query_weight, key_weight, value_weight, gate_weight, decay_matrix,
            decay_offset_bias, head_gain, out_weight, mixer_gain, up_weight, down_weight,
        )
    seq_count = block_state.shape[0]
    head_count = block_state.shape[1]
    span_size = key_cache.shape[2]
    whole_rows = tokens.astype(jnp.float32)
    square_sum = jnp.sum(whole_rows * whole_rows, axis=1)
    scaled = (whole_rows * attn_gain).astype(jnp.bfloat16)
    query_part = jnp.dot(scaled, query_weight, preferred_element_type=jnp.float32)
    key_part = jnp.dot(scaled, key_weight, preferred_element_type=jnp.float32)
    value_part = jnp.dot(scaled, value_weight, preferred_element_type=jnp.float32)
    gate_part = jnp.dot(scaled, gate_weight, preferred_element_type=jnp.float32)
    decay_part = jnp.dot(scaled, decay_matrix, preferred_element_type=jnp.float32)
    square_total = lax.psum(square_sum, "kv")
    query_sum, key_sum, value_sum, gate_sum, decay_running_sum = (
        lax.psum_scatter(query_part, "kv", scatter_dimension=0, tiled=True),
        lax.psum_scatter(key_part, "kv", scatter_dimension=0, tiled=True),
        lax.psum_scatter(value_part, "kv", scatter_dimension=0, tiled=True),
        lax.psum_scatter(gate_part, "kv", scatter_dimension=0, tiled=True),
        lax.psum_scatter(decay_part, "kv", scatter_dimension=0, tiled=True),
    )
    own_square = lax.dynamic_slice_in_dim(square_total, lax.axis_index("kv") * seq_count, seq_count)
    scale_per_row = lax.rsqrt(own_square / D + NORM_EPS)[:, None]
    query = (query_sum * scale_per_row * KEY_WIDTH ** (-0.5)).reshape(
        seq_count, head_count, KEY_WIDTH
    )
    key_new = (key_sum * scale_per_row).reshape(seq_count, head_count, KEY_WIDTH)
    value_new = (value_sum * scale_per_row).reshape(seq_count, head_count, DV)
    gate = gate_sum * scale_per_row
    logarithm_decay = (
        jax.nn.log_sigmoid(decay_running_sum * scale_per_row + decay_offset_bias) / DECAY_SOFTNESS
    )
    token_place = lax.broadcasted_iota(jnp.int32, (1, 1, span_size), 2)
    lengths_now = span_lengths[:, None, None]
    previous = jnp.sum(jnp.where(token_place == lengths_now - 2, decay_cache, 0.0), axis=-1)
    now_decay = (previous + logarithm_decay).reshape(seq_count, head_count, KEY_WIDTH)
    decays_span = decay_cache.reshape(seq_count, head_count, KEY_WIDTH, span_size)
    in_use = (token_place < lengths_now - 1)[:, :, None, :]
    factor = jnp.where(in_use, jnp.exp(now_decay[..., None] - decays_span), 0.0)
    keys_span = key_cache.reshape(seq_count, head_count, KEY_WIDTH, span_size)
    scores = jnp.sum(query[..., None] * keys_span.astype(jnp.float32) * factor, axis=2)
    scores_low = scores.astype(jnp.bfloat16)
    values_span = value_cache.reshape(seq_count, head_count, DV, span_size)
    history = jnp.einsum(
        "nhs,nhvs->nhv", scores_low, values_span, preferred_element_type=jnp.float32
    )
    carried = jnp.einsum(
        "nhc,nhcv->nhv", query * jnp.exp(now_decay), block_state, precision=lax.Precision.HIGHEST
    )
    own_term = jnp.sum(query * key_new, axis=-1, keepdims=True) * value_new
    raw = carried + history + own_term
    normed = raw * lax.rsqrt(jnp.mean(raw * raw, axis=-1, keepdims=True) + NORM_EPS) * head_gain
    mixed = (normed.reshape(seq_count, head_count * DV) * jax.nn.silu(gate)).astype(jnp.bfloat16)
    attn_terms = jnp.dot(
        lax.all_gather(mixed, "kv", axis=0, tiled=True),
        out_weight,
        preferred_element_type=jnp.float32,
    )
    attn_out = lax.psum(attn_terms, "tp")
    resid = (whole_rows + attn_out).astype(jnp.bfloat16)
    resid_rows = resid.astype(jnp.float32)
    mixer_square = jnp.sum(resid_rows * resid_rows, axis=1)
    mixer_scaled = (resid_rows * mixer_gain).astype(jnp.bfloat16)
    up_part = jnp.dot(mixer_scaled, up_weight, preferred_element_type=jnp.float32)
    up_share, square_share = (
        lax.psum_scatter(up_part, "kv", scatter_dimension=0, tiled=True),
        lax.psum_scatter(mixer_square, "kv", scatter_dimension=0, tiled=True),
    )
    hidden_share = jnp.square(
        jax.nn.relu(up_share * lax.rsqrt(square_share / D + NORM_EPS)[:, None])
    )
    hidden_share = hidden_share.astype(jnp.bfloat16)
    down_terms = jnp.dot(
        lax.all_gather(hidden_share, "kv", axis=0, tiled=True),
        down_weight,
        preferred_element_type=jnp.float32,
    )
    mixer_out = lax.psum(down_terms, "tp")
    return (resid_rows + mixer_out).astype(jnp.bfloat16)


def solution(mesh):
    placed = (
        P("grp", "kv"),
        P(("grp", "kv")),
        P(("grp", "kv"), "tp", None, None),
        P(("grp", "kv"), "tp", None),
        P(("grp", "kv"), "tp", None),
        P(("grp", "kv"), "tp", None),
        P("kv"),
        P("kv", "tp"),
        P("kv", "tp"),
        P("kv", "tp"),
        P("kv", "tp"),
        P("kv", "tp"),
        P("tp"),
        P(),
        P("tp", "kv"),
        P("kv"),
        P("kv", "tp"),
        P("tp", "kv"),
    )
    return jax.shard_map(
        shards, mesh=mesh, in_specs=placed, out_specs=P("grp", "kv"), check_vma=False
    )
```

```python
import functools

import jax
import jax.numpy as jnp
from jax import lax
from jax.experimental import pallas as pl
from jax.experimental.pallas import tpu as pltpu
from jax.sharding import PartitionSpec as P

D = 4096
KEY_WIDTH = 32
DV = 64


NORM_EPS = 1e-06
DECAY_SOFTNESS = 16.0
MESH = pl.DeviceIdType.MESH
LANES = 128
F32 = jnp.float32
BF16 = jnp.bfloat16


def greet(axes):
    barrier = pltpu.get_barrier_semaphore()
    count = 0
    for axis in axes:
        size = lax.axis_size(axis)
        me = lax.axis_index(axis)
        for step in range(1, size):
            pl.semaphore_signal(
                barrier, inc=1, device_id={axis: lax.rem(me + step, size)}, device_id_type=MESH
            )
        count += size - 1
    pl.semaphore_wait(barrier, count)


def send(axis, step, src, dst, send_sem, recv_sem):
    size = lax.axis_size(axis)
    peer = lax.rem(lax.axis_index(axis) + step, size)
    copy = pltpu.make_async_remote_copy(
        src_ref=src(peer),
        dst_ref=dst,
        send_sem=send_sem,
        recv_sem=recv_sem,
        device_id={axis: peer},
        device_id_type=MESH,
    )
    copy.start()
    return copy


def project_kernel(
    parts, tok_ref, gain_ref, *refs
):
    weights, refs = refs[:5], refs[5:]
    sum_ref, sq_ref = refs[:2]
    wbuf, part, outgoing, incoming, sq_out, sq_in, wsem, ssem, rsem, qssem, qrsem = refs[2:]
    n, rows = outgoing.shape[0], outgoing.shape[1]
    me = lax.axis_index("kv")
    loads = []
    for i, (which, col, place, width) in enumerate(parts):
        load = pltpu.make_async_copy(
            weights[which].at[:, pl.ds(col, width)], wbuf.at[:, pl.ds(place, width)], wsem.at[i]
        )
        load.start()
        loads.append(load)
    x = tok_ref[...].astype(F32)
    scaled = (x * gain_ref[...]).astype(BF16)
    square = jnp.sum(x * x, axis=1, keepdims=True)
    sq_out[...] = jnp.broadcast_to(square, (x.shape[0], LANES)).reshape(sq_out.shape)
    greet(("kv",))
    copies = []
    for k in range(1, n):
        copies.append(
            send("kv", k, lambda p: sq_out.at[p], sq_in.at[k - 1], qssem.at[k - 1], qrsem.at[k - 1])
        )
    for i, (which, col, place, width) in enumerate(parts):
        loads[i].wait()
        cols = pl.ds(place, width)
        got = jnp.dot(scaled, wbuf[:, cols], preferred_element_type=F32).reshape(n, rows, width)
        part[:, :, cols] = got
        outgoing[:, :, cols] = got.astype(BF16)
        for k in SEND_ORDER(n):
            copies.append(
                send(
                    "kv",
                    k,
                    lambda p: outgoing.at[p, :, cols],
                    incoming.at[k - 1, :, cols],
                    ssem.at[k - 1, i],
                    rsem.at[k - 1, i],
                )
            )
    for copy in copies:
        copy.wait_recv()
    total = part[me]
    square = sq_out[me]
    for k in range(n - 1):
        total = total + incoming[k].astype(F32)
        square = square + sq_in[k]
    sum_ref[...] = total
    sq_ref[...] = square
    for copy in copies:
        copy.wait_send()


def SEND_ORDER(n):
    return sorted(range(1, n), key=lambda k: -min(k, n - k))


def project(tokens, gain, weights):
    n = lax.axis_size("kv")
    rows = tokens.shape[0] // n
    parts, place = [], 0
    for which, w in enumerate(weights):
        width = min(512, w.shape[1])
        for col in range(0, w.shape[1], width):
            parts.append((which, col, place, width))
            place += width
    vmem = pl.BlockSpec(memory_space=pltpu.VMEM)
    return pl.pallas_call(
        functools.partial(project_kernel, parts),
        out_shape=(
            jax.ShapeDtypeStruct((rows, place), F32),
            jax.ShapeDtypeStruct((rows, LANES), F32),
        ),
        in_specs=[vmem, vmem] + [pl.BlockSpec(memory_space=pltpu.HBM)] * 5,
        out_specs=(vmem, vmem),
        scratch_shapes=[
            pltpu.VMEM((tokens.shape[1], place), BF16),
            pltpu.VMEM((n, rows, place), F32),
            pltpu.VMEM((n, rows, place), BF16),
            pltpu.VMEM((n - 1, rows, place), BF16),
            pltpu.VMEM((n, rows, LANES), F32),
            pltpu.VMEM((n - 1, rows, LANES), F32),
            pltpu.SemaphoreType.DMA((len(parts),)),
            pltpu.SemaphoreType.DMA((n - 1, len(parts))),
            pltpu.SemaphoreType.DMA((n - 1, len(parts))),
            pltpu.SemaphoreType.DMA((n - 1,)),
            pltpu.SemaphoreType.DMA((n - 1,)),
        ],
        compiler_params=pltpu.CompilerParams(
            collective_id=0, has_side_effects=True, vmem_limit_bytes=62 << 20
        ),
        name="project",
    )(tokens, gain.reshape(1, -1), *weights)


NT = (((1,), (1,)), ((), ()))


def attend_kernel(
    len_ref, last_ref, sum_ref, sq_ref, bias_ref, hg_ref, k1, k2a, k2b, d1, d2a, d2b,
    v1, v2a, v2b, st, out_ref, q_t, ld_t, qk_t, vn, gs, now_s, q_s, hist, raw,
):
    step = pl.program_id(0)
    rows = out_ref.shape[0]
    heads = st.shape[1]
    keys, vals = heads * KEY_WIDTH, heads * DV
    lane = lax.broadcasted_iota(jnp.int32, (1, LANES), 1)

    @pl.when(step == 0)
    def _():
        scale = lax.rsqrt(sq_ref[:, :1] / D + NORM_EPS)
        q = sum_ref[:, :keys] * scale * KEY_WIDTH ** (-0.5)
        key_new = sum_ref[:, keys : 2 * keys] * scale
        at = 2 * keys
        vn[...] = sum_ref[:, at : at + vals] * scale
        g = sum_ref[:, at + vals : at + 2 * vals] * scale
        gs[...] = g * (1.0 / (1.0 + jnp.exp(-g))) * jnp.concatenate([hg_ref[...]] * heads, axis=1)
        x = sum_ref[:, at + 2 * vals :] * scale + bias_ref[...]
        ld = (jnp.minimum(x, 0.0) - jnp.log1p(jnp.exp(-jnp.abs(x)))) / DECAY_SOFTNESS
        spare = jnp.zeros((LANES - rows, keys), F32)
        q_t[...] = jnp.concatenate([q, spare], axis=0).T
        ld_t[...] = jnp.concatenate([ld, spare], axis=0).T
        pick = lax.broadcasted_iota(jnp.int32, (heads, keys), 1) // KEY_WIDTH
        pick = (pick == lax.broadcasted_iota(jnp.int32, (heads, keys), 0)).astype(F32)
        qk_t[...] = lax.dot_general(
            pick,
            jnp.concatenate([q * key_new, spare], axis=0),
            NT,
            precision=lax.Precision.HIGHEST,
            preferred_element_type=F32,
        )

    seconds = ((k2a, d2a, v2a), (k2b, d2b, v2b))
    lengths = [len_ref[2 * step + j] for j in range(2)]
    mine = [lane == 2 * step + j for j in range(2)]
    wide = (keys, LANES)

    def block(j, k, d, v, offset):
        s = k.astype(F32) * q_s[j] * jnp.exp(now_s[j] - d)
        s = jnp.sum(s.reshape(heads, KEY_WIDTH, LANES), axis=1)
        s = jnp.where(lane + offset < lengths[j] - 1, s, 0.0).astype(BF16)
        return lax.dot_general(s, v, NT, preferred_element_type=F32)

    for j in range(2):
        prev = jnp.where(lane == lengths[j] - 2, d1[j], 0.0)
        prev = prev + jnp.where(lane + LANES == lengths[j] - 2, seconds[j][1][0], 0.0)
        own_decay = jnp.where(mine[j], ld_t[...], 0.0)
        now_s[j] = jnp.broadcast_to(jnp.sum(prev + own_decay, axis=1, keepdims=True), wide)
        q = jnp.sum(jnp.where(mine[j], q_t[...], 0.0), axis=1, keepdims=True)
        q_s[j] = jnp.broadcast_to(q, wide)
    for j in range(2):
        hist[j] = block(j, k1[j], d1[j], v1[j], 0)
    for j in range(2):

        @pl.when(lengths[j] - 1 > LANES)
        def _(j=j):
            k2, d2, v2 = seconds[j]
            hist[j] += block(j, k2[0], d2[0], v2[0], LANES)

    own = lax.broadcasted_iota(jnp.int32, (heads, vals), 1) // DV
    own = own == lax.broadcasted_iota(jnp.int32, (heads, vals), 0)
    for j in range(2):
        weight = (q_s[j] * jnp.exp(now_s[j]))[:, :DV]
        carried = weight * st[j].reshape(keys, DV)
        carried = jnp.sum(carried.reshape(heads, KEY_WIDTH, DV), axis=1)
        carried = jnp.concatenate([carried] * heads, axis=1)
        qk = jnp.sum(jnp.where(mine[j], qk_t[...], 0.0), axis=1, keepdims=True)
        row = pl.ds(2 * step + j, 1)
        whole = hist[j] + carried + qk * vn[row, :]
        whole = jnp.where(own, whole, 0.0)
        mean = jnp.sum(whole * whole, axis=1, keepdims=True) / DV
        whole = whole * lax.rsqrt(mean + NORM_EPS)
        raw[row, :] = jnp.sum(whole, axis=0, keepdims=True)

    @pl.when(step == pl.num_programs(0) - 1)
    def _():
        out_ref[...] = (raw[...] * gs[...]).astype(BF16)


def attend(span_lengths, sums, square, bias, head_gain, keys, values, decays, state):
    rows, heads = state.shape[:2]
    kw, vw = heads * KEY_WIDTH, heads * DV
    order = jnp.arange(rows, dtype=jnp.int32)
    needed = jnp.where(span_lengths - 1 > LANES, order, order % 2)
    before = (order[None, :] <= order[:, None]) & (order[None, :] % 2 == order[:, None] % 2)
    last = jnp.max(jnp.where(before, needed[None, :], 0), axis=1)

    def first(width):
        return pl.BlockSpec((2, width, LANES), lambda i, ln, la: (i, 0, 0))

    def second(width, j):
        return pl.BlockSpec((1, width, LANES), lambda i, ln, la: (la[2 * i + j], 0, 1))

    def fixed(shape):
        return pl.BlockSpec(shape, lambda i, ln, la: (0,) * len(shape))

    return pl.pallas_call(
        attend_kernel,
        out_shape=jax.ShapeDtypeStruct((rows, vw), BF16),
        grid_spec=pltpu.PrefetchScalarGridSpec(
            num_scalar_prefetch=2,
            grid=(rows // 2,),
            in_specs=[
                fixed(sums.shape),
                fixed(square.shape),
                fixed((1, kw)),
                fixed((1, DV)),
                first(kw),
                second(kw, 0),
                second(kw, 1),
                first(kw),
                second(kw, 0),
                second(kw, 1),
                first(vw),
                second(vw, 0),
                second(vw, 1),
                pl.BlockSpec((2, heads, KEY_WIDTH, DV), lambda i, ln, la: (i, 0, 0, 0)),
            ],
            out_specs=fixed((rows, vw)),
            scratch_shapes=[
                pltpu.VMEM((kw, LANES), F32),
                pltpu.VMEM((kw, LANES), F32),
                pltpu.VMEM((heads, LANES), F32),
                pltpu.VMEM((rows, vw), F32),
                pltpu.VMEM((rows, vw), F32),
                pltpu.VMEM((2, kw, LANES), F32),
                pltpu.VMEM((2, kw, LANES), F32),
                pltpu.VMEM((2, heads, vw), F32),
                pltpu.VMEM((rows, vw), F32),
            ],
        ),
        compiler_params=pltpu.CompilerParams(
            dimension_semantics=("arbitrary",), vmem_limit_bytes=62 << 20
        ),
        name="attend",
    )(
        span_lengths, last, sums, square, bias.reshape(1, -1), head_gain.reshape(1, -1),
        keys, keys, keys, decays, decays, decays, values, values, values, state,
    )


def finish_kernel(
    mixed_ref, tok_ref, gain_ref, ow_ref, uw_ref, dw_ref, out_ref,
    ow, uw, dw, gath, part, t_out, t_in, resid, scaled, sq_out, sq_in,
    u_part, u_own, u_out, u_in, hid, total, t_out2, t_in2, done,
    wsem, g_s, g_r, a_s, a_r, b_s, b_r, q_s, q_r, u_s, u_r, h_s, h_r, c_s, c_r, e_s, e_r,
):
    n, m = lax.axis_size("kv"), lax.axis_size("tp")
    me, col = lax.axis_index("kv"), lax.axis_index("tp")
    chunks = u_s.shape[1]
    width = u_out.shape[2] // chunks
    loads = [
        pltpu.make_async_copy(ow_ref, ow, wsem.at[0]),
    ]
    for c in range(chunks):
        at = pl.ds(c * width, width)
        loads.append(pltpu.make_async_copy(uw_ref.at[:, at], uw.at[:, at], wsem.at[1 + c]))
    loads.append(pltpu.make_async_copy(dw_ref, dw, wsem.at[1 + chunks]))
    for load in loads:
        load.start()
    greet(("kv", "tp"))
    copies = []

    def wait_all(group):
        for copy in group:
            copy.wait_recv()
        copies.extend(group)

    group = [
        send("kv", k, lambda p: mixed_ref, gath.at[me], g_s.at[k - 1], g_r.at[k - 1])
        for k in SEND_ORDER(n)
    ]
    gath[me] = mixed_ref[...]
    wait_all(group)
    loads[0].wait()
    rows = gath.shape[0] * gath.shape[1]

    def over_tp(value, outgoing, incoming, ss, rs):
        part[...] = value.reshape(part.shape)
        outgoing[...] = value.reshape(part.shape).astype(BF16)
        group = [
            send("tp", k, lambda p: outgoing.at[p], incoming.at[k - 1], ss.at[k - 1], rs.at[k - 1])
            for k in range(1, m)
        ]
        wait_all(group)
        result = part[col]
        for k in range(m - 1):
            result = result + incoming[k].astype(F32)
        return result

    def to_tp(buffer, ss, rs):
        group = [
            send("tp", k, lambda p: buffer.at[col], buffer.at[col], ss.at[k - 1], rs.at[k - 1])
            for k in range(1, m)
        ]
        wait_all(group)

    x = gath[...].reshape(rows, gath.shape[2])
    attn = over_tp(jnp.dot(x, ow[...], preferred_element_type=F32), t_out, t_in, a_s, a_r)
    resid[col] = (tok_ref[col].astype(F32) + attn).astype(BF16)
    to_tp(resid, b_s, b_r)
    whole = resid[...].reshape(rows, resid.shape[2]).astype(F32)
    square = jnp.sum(whole * whole, axis=1, keepdims=True)
    sq_out[...] = jnp.broadcast_to(square, (rows, LANES)).reshape(sq_out.shape)
    sq_group = [
        send("kv", k, lambda p: sq_out.at[p], sq_in.at[k - 1], q_s.at[k - 1], q_r.at[k - 1])
        for k in SEND_ORDER(n)
    ]
    scaled[...] = (whole * gain_ref[...]).astype(BF16)

    def toward(bit, ref, ss, rs):
        peer = me + bit - 2 * bit * (me // bit % 2)
        copy = pltpu.make_async_remote_copy(
            src_ref=ref(peer), dst_ref=ref(peer), send_sem=ss, recv_sem=rs,
            device_id={"kv": peer}, device_id_type=MESH,
        )
        copy.start()
        return copy

    groups = []
    for c in range(chunks):
        at = pl.ds(c * width, width)
        loads[1 + c].wait()
        got = jnp.dot(scaled[...], uw[:, at], preferred_element_type=F32)
        got = got.reshape(u_part.shape)
        u_part[...] = got
        u_out[:, :, at] = got.astype(BF16)
        groups.append(
            [
                send(
                    "kv", k, lambda p: u_out.at[p, :, at], u_in.at[k - 1, :, at],
                    u_s.at[k - 1, c], u_r.at[k - 1, c],
                )
                for k in SEND_ORDER(n)
            ]
        )
        u_own[:, at] = u_part[me]
    wait_all(sq_group)
    square = sq_out[me]
    for k in range(n - 1):
        square = square + sq_in[k]
    scale = lax.rsqrt(square[:, :1] / D + NORM_EPS)
    hidden_groups = []
    for c in range(chunks):
        at = pl.ds(c * width, width)
        wait_all(groups[c])
        got = u_own[:, at]
        for k in range(n - 1):
            got = got + u_in[k, :, at].astype(F32)
        hid[me, :, at] = jnp.square(jnp.maximum(got * scale, 0.0)).astype(BF16)
        hidden_groups.append(
            [
                toward(2, lambda p: hid.at[me, :, at], h_s.at[0, c], h_r.at[0, c]),
                toward(1, lambda p: hid.at[me, :, at], h_s.at[1, c], h_r.at[1, c]),
            ]
        )
    for c in range(chunks):
        at = pl.ds(c * width, width)
        wait_all(hidden_groups[c][:1])
        far = me + 2 - 4 * (me // 2)
        hidden_groups[c].append(
            toward(1, lambda p: hid.at[far, :, at], h_s.at[2, c], h_r.at[2, c])
        )
    loads[1 + chunks].wait()
    for c in range(chunks):
        at = pl.ds(c * width, width)
        wait_all(hidden_groups[c][1:])
        got = jnp.dot(
            hid[:, :, at].reshape(rows, width), dw[at, :], preferred_element_type=F32
        )
        if c == 0:
            total[...] = got
        else:
            total[...] += got
    mixer = over_tp(total[...], t_out2, t_in2, c_s, c_r)
    done[col] = (resid[col].astype(F32) + mixer).astype(BF16)
    to_tp(done, e_s, e_r)
    out_ref[...] = done[...]
    for copy in copies:
        copy.wait_send()


def finish(mixed, tokens, gain, out_weight, up_weight, down_weight):
    n, m = lax.axis_size("kv"), lax.axis_size("tp")
    rows, feats = tokens.shape
    vals, hidden = out_weight.shape[0], up_weight.shape[1]
    own, share = rows // n, rows // m
    chunks = 4
    vmem = pl.BlockSpec(memory_space=pltpu.VMEM)
    hbm = pl.BlockSpec(memory_space=pltpu.HBM)
    dma = pltpu.SemaphoreType.DMA
    out = pl.pallas_call(
        finish_kernel,
        out_shape=jax.ShapeDtypeStruct((m, share, feats), BF16),
        in_specs=[vmem, vmem, vmem, hbm, hbm, hbm],
        out_specs=vmem,
        scratch_shapes=[
            pltpu.VMEM(out_weight.shape, BF16),
            pltpu.VMEM(up_weight.shape, BF16),
            pltpu.VMEM(down_weight.shape, BF16),
            pltpu.VMEM((n, own, vals), BF16),
            pltpu.VMEM((m, share, feats), F32),
            pltpu.VMEM((m, share, feats), BF16),
            pltpu.VMEM((m - 1, share, feats), BF16),
            pltpu.VMEM((m, share, feats), BF16),
            pltpu.VMEM((rows, feats), BF16),
            pltpu.VMEM((n, own, LANES), F32),
            pltpu.VMEM((n - 1, own, LANES), F32),
            pltpu.VMEM((n, own, hidden // chunks), F32),
            pltpu.VMEM((own, hidden), F32),
            pltpu.VMEM((n, own, hidden), BF16),
            pltpu.VMEM((n - 1, own, hidden), BF16),
            pltpu.VMEM((n, own, hidden), BF16),
            pltpu.VMEM((rows, feats), F32),
            pltpu.VMEM((m, share, feats), BF16),
            pltpu.VMEM((m - 1, share, feats), BF16),
            pltpu.VMEM((m, share, feats), BF16),
            dma((2 + chunks,)),
            dma((n - 1,)),
            dma((n - 1,)),
            dma((m - 1,)),
            dma((m - 1,)),
            dma((m - 1,)),
            dma((m - 1,)),
            dma((n - 1,)),
            dma((n - 1,)),
            dma((n - 1, chunks)),
            dma((n - 1, chunks)),
            dma((n - 1, chunks)),
            dma((n - 1, chunks)),
            dma((m - 1,)),
            dma((m - 1,)),
            dma((m - 1,)),
            dma((m - 1,)),
        ],
        compiler_params=pltpu.CompilerParams(
            collective_id=1, has_side_effects=True, vmem_limit_bytes=62 << 20
        ),
        name="finish",
    )(
        mixed, tokens.reshape(m, share, feats), gain.reshape(1, -1),
        out_weight, up_weight, down_weight,
    )
    return out.reshape(rows, feats)


def kernel_shards(
    tokens,
    span_lengths,
    block_state,
    key_cache,
    value_cache,
    decay_cache,
    attn_gain,
    query_weight,
    key_weight,
    value_weight,
    gate_weight,
    decay_matrix,
    decay_offset_bias,
    head_gain,
    out_weight,
    mixer_gain,
    up_weight,
    down_weight,
):
    weights = (query_weight, key_weight, value_weight, gate_weight, decay_matrix)
    sums, square = project(tokens, attn_gain, weights)
    mixed = attend(
        span_lengths, sums, square, decay_offset_bias, head_gain,
        key_cache, value_cache, decay_cache, block_state,
    )
    return finish(mixed, tokens, mixer_gain, out_weight, up_weight, down_weight)


def fits(tokens, block_state, key_cache):
    rows, heads = block_state.shape[:2]
    share = tokens.shape[0] // lax.axis_size("tp")
    return (
        lax.axis_size("kv") == 4
        and rows % 16 == 0
        and share % 16 == 0
        and heads % 8 == 0
        and rows < LANES
        and key_cache.shape[2] == 2 * LANES
    )


def shards(
    tokens,
    span_lengths,
    block_state,
    key_cache,
    value_cache,
    decay_cache,
    attn_gain,
    query_weight,
    key_weight,
    value_weight,
    gate_weight,
    decay_matrix,
    decay_offset_bias,
    head_gain,
    out_weight,
    mixer_gain,
    up_weight,
    down_weight,
):
    if fits(tokens, block_state, key_cache):
        return kernel_shards(
            tokens, span_lengths, block_state, key_cache, value_cache, decay_cache,
            attn_gain, query_weight, key_weight, value_weight, gate_weight, decay_matrix,
            decay_offset_bias, head_gain, out_weight, mixer_gain, up_weight, down_weight,
        )
    seq_count = block_state.shape[0]
    head_count = block_state.shape[1]
    span_size = key_cache.shape[2]
    whole_rows = tokens.astype(jnp.float32)
    square_sum = jnp.sum(whole_rows * whole_rows, axis=1)
    scaled = (whole_rows * attn_gain).astype(jnp.bfloat16)
    query_part = jnp.dot(scaled, query_weight, preferred_element_type=jnp.float32)
    key_part = jnp.dot(scaled, key_weight, preferred_element_type=jnp.float32)
    value_part = jnp.dot(scaled, value_weight, preferred_element_type=jnp.float32)
    gate_part = jnp.dot(scaled, gate_weight, preferred_element_type=jnp.float32)
    decay_part = jnp.dot(scaled, decay_matrix, preferred_element_type=jnp.float32)
    square_total = lax.psum(square_sum, "kv")
    query_sum, key_sum, value_sum, gate_sum, decay_running_sum = (
        lax.psum_scatter(query_part, "kv", scatter_dimension=0, tiled=True),
        lax.psum_scatter(key_part, "kv", scatter_dimension=0, tiled=True),
        lax.psum_scatter(value_part, "kv", scatter_dimension=0, tiled=True),
        lax.psum_scatter(gate_part, "kv", scatter_dimension=0, tiled=True),
        lax.psum_scatter(decay_part, "kv", scatter_dimension=0, tiled=True),
    )
    own_square = lax.dynamic_slice_in_dim(square_total, lax.axis_index("kv") * seq_count, seq_count)
    scale_per_row = lax.rsqrt(own_square / D + NORM_EPS)[:, None]
    query = (query_sum * scale_per_row * KEY_WIDTH ** (-0.5)).reshape(
        seq_count, head_count, KEY_WIDTH
    )
    key_new = (key_sum * scale_per_row).reshape(seq_count, head_count, KEY_WIDTH)
    value_new = (value_sum * scale_per_row).reshape(seq_count, head_count, DV)
    gate = gate_sum * scale_per_row
    logarithm_decay = (
        jax.nn.log_sigmoid(decay_running_sum * scale_per_row + decay_offset_bias) / DECAY_SOFTNESS
    )
    token_place = lax.broadcasted_iota(jnp.int32, (1, 1, span_size), 2)
    lengths_now = span_lengths[:, None, None]
    previous = jnp.sum(jnp.where(token_place == lengths_now - 2, decay_cache, 0.0), axis=-1)
    now_decay = (previous + logarithm_decay).reshape(seq_count, head_count, KEY_WIDTH)
    decays_span = decay_cache.reshape(seq_count, head_count, KEY_WIDTH, span_size)
    in_use = (token_place < lengths_now - 1)[:, :, None, :]
    factor = jnp.where(in_use, jnp.exp(now_decay[..., None] - decays_span), 0.0)
    keys_span = key_cache.reshape(seq_count, head_count, KEY_WIDTH, span_size)
    scores = jnp.sum(query[..., None] * keys_span.astype(jnp.float32) * factor, axis=2)
    scores_low = scores.astype(jnp.bfloat16)
    values_span = value_cache.reshape(seq_count, head_count, DV, span_size)
    history = jnp.einsum(
        "nhs,nhvs->nhv", scores_low, values_span, preferred_element_type=jnp.float32
    )
    carried = jnp.einsum(
        "nhc,nhcv->nhv", query * jnp.exp(now_decay), block_state, precision=lax.Precision.HIGHEST
    )
    own_term = jnp.sum(query * key_new, axis=-1, keepdims=True) * value_new
    raw = carried + history + own_term
    normed = raw * lax.rsqrt(jnp.mean(raw * raw, axis=-1, keepdims=True) + NORM_EPS) * head_gain
    mixed = (normed.reshape(seq_count, head_count * DV) * jax.nn.silu(gate)).astype(jnp.bfloat16)
    attn_terms = jnp.dot(
        lax.all_gather(mixed, "kv", axis=0, tiled=True),
        out_weight,
        preferred_element_type=jnp.float32,
    )
    attn_out = lax.psum(attn_terms, "tp")
    resid = (whole_rows + attn_out).astype(jnp.bfloat16)
    resid_rows = resid.astype(jnp.float32)
    mixer_square = jnp.sum(resid_rows * resid_rows, axis=1)
    mixer_scaled = (resid_rows * mixer_gain).astype(jnp.bfloat16)
    up_part = jnp.dot(mixer_scaled, up_weight, preferred_element_type=jnp.float32)
    up_share, square_share = (
        lax.psum_scatter(up_part, "kv", scatter_dimension=0, tiled=True),
        lax.psum_scatter(mixer_square, "kv", scatter_dimension=0, tiled=True),
    )
    hidden_share = jnp.square(
        jax.nn.relu(up_share * lax.rsqrt(square_share / D + NORM_EPS)[:, None])
    )
    hidden_share = hidden_share.astype(jnp.bfloat16)
    down_terms = jnp.dot(
        lax.all_gather(hidden_share, "kv", axis=0, tiled=True),
        down_weight,
        preferred_element_type=jnp.float32,
    )
    mixer_out = lax.psum(down_terms, "tp")
    return (resid_rows + mixer_out).astype(jnp.bfloat16)


def solution(mesh):
    placed = (
        P("grp", "kv"),
        P(("grp", "kv")),
        P(("grp", "kv"), "tp", None, None),
        P(("grp", "kv"), "tp", None),
        P(("grp", "kv"), "tp", None),
        P(("grp", "kv"), "tp", None),
        P("kv"),
        P("kv", "tp"),
        P("kv", "tp"),
        P("kv", "tp"),
        P("kv", "tp"),
        P("kv", "tp"),
        P("tp"),
        P(),
        P("tp", "kv"),
        P("kv"),
        P("kv", "tp"),
        P("tp", "kv"),
    )
    return jax.shard_map(
        shards, mesh=mesh, in_specs=placed, out_specs=P("grp", "kv"), check_vma=False
    )
```
